512 devices in a mesh: grp: 2 (over y), fs: 16 (over z), tp: 16 (over x, core).
Axes of the slice: x: 8, y: 2, z: 16, core: 2. Of those that a mesh axis runs over, the one named last changes fastest.
The devices are a block of a 8x16x16 slice.
Arguments:
- tokens: bfloat16 [16384, 2048], P(('grp', 'fs')), parts along dimension 0, may hold values from -6 to 6
- pre_gain: float32 [2048], replicated, may hold values from 0.1 to 1.9
- gate_weight: float32 [2048, 5632], P('fs', 'tp'), may hold values from -0.125 to 0.125
- gate_scale: float32 [5632], P('tp'), may hold values from 0.5 to 2
- up_weight: float32 [2048, 5632], P('fs', 'tp'), may hold values from -0.125 to 0.125
- up_scale: float32 [5632], P('tp'), may hold values from 0.5 to 2
- down_weight: float32 [5632, 2048], P('tp', 'fs'), may hold values from -0.078125 to 0.078125
- down_scale: float32 [2048], replicated, may hold values from 0.3 to 3
- post_gain: float32 [2048], replicated, may hold values from 0.1 to 1.9
Outputs:
- mixed: bfloat16 [16384, 2048], P(('grp', 'fs')), parts along dimension 0
The draws below stay inside these ranges and needn't reach their ends.
There are 2 independent parts, one for each index of `grp`. The reference program is written for one: setup_inputs(seed, part) draws one part's arguments, and reference() takes and returns one part's arrays. A program takes and returns all parts, laid end to end along the dimension named above; an argument that names none is the same for every part. Nothing has to cross between parts.
All inputs are finite; a program needn't handle non-finite values.
Results may differ from the reference program's by a relative error of at most 0.018.
Values may be sent and summed in bfloat16 or wider, within the bound.
No kernel may reach another device: no remote copies, remote signals or barrier semaphores. Data moves between devices by JAX's collectives and lax.ppermute only.
A program may use at most 64 MiB of HBM per device.

```python
import math
import jax
import jax.numpy as jnp
from jax import lax

D = 2048
FF = 5632
TOKENS = 8192
N_TP = 16


def shard_levels(stream_key, dims, pieces, least, high):
    def one(dim, shards_of):
        draws = jax.random.uniform(jax.random.fold_in(jax.random.fold_in(stream_key, 6), dim), (shards_of,), jnp.float32, least / len(pieces), high / len(pieces))
        return jnp.repeat(jnp.exp(draws), dims[dim] // shards_of).reshape((-1,) + (1,) * (len(dims) - dim - 1))

    level = one(*pieces[0])
    for cut in pieces[1:]:
        level = level * one(*cut)
    return level


def bell_draw(key, shape, scale, reach, shards=(), held_as=jnp.bfloat16):
    factor_of = shard_levels(key, shape, shards, -0.22, 0.18) if shards else 1.0
    array = jax.random.normal(key, shape, jnp.float32) * scale * factor_of
    return jnp.minimum(jnp.maximum(array, -reach), reach).astype(held_as)


def setup_inputs(seed: int = 0, part: int = 0) -> dict:
    splits = jax.random.split(jax.random.key(seed), 10)
    part_keys = jax.random.split(jax.random.fold_in(splits[9], part), 10)
    return {
        "tokens": bell_draw(part_keys[0], (TOKENS, D), 1.0, 6.0, ((0, 16),)),
        "pre_gain": jnp.clip(1.0 + 0.18 * jax.random.normal(splits[1], (D,), jnp.float32), 0.1, 1.9),
        "gate_weight": bell_draw(splits[2], (D, FF), D ** -0.5, 0.125, ((0, 16), (1, 16)), jnp.float32),
        "gate_scale": jnp.clip(jnp.exp(math.log(2.0) - 1.3862944 * jax.random.uniform(splits[3], (FF,), jnp.float32) ** shard_levels(splits[3], (FF,), ((0, 16),), -0.2, 0.2)), 0.5, 2.0),
        "up_weight": bell_draw(splits[4], (D, FF), D ** -0.5, 0.125, ((0, 16), (1, 16)), jnp.float32),
        "up_scale": jnp.clip(jnp.exp(math.log(2.0) - 1.3862944 * jax.random.uniform(splits[5], (FF,), jnp.float32) ** shard_levels(splits[5], (FF,), ((0, 16),), -0.2, 0.2)), 0.5, 2.0),
        "down_weight": bell_draw(splits[6], (FF, D), FF ** -0.5, 0.078125, ((0, 16), (1, 16)), jnp.float32),
        "down_scale": jnp.clip(jnp.exp(jax.random.uniform(splits[7], (D,), jnp.float32, math.log(0.3), math.log(3.0))), 0.3, 3.0),
        "post_gain": jnp.clip(1.0 + 0.18 * jax.random.normal(splits[8], (D,), jnp.float32), 0.1, 1.9),
    }


EPS = 1e-06

def reference(tokens, pre_gain, gate_weight, gate_scale, up_weight, up_scale, down_weight, down_scale, post_gain):
    rows = tokens.astype(jnp.float32)
    normed = (rows * lax.rsqrt(lax.optimization_barrier(jnp.mean(rows * rows, axis=-1, keepdims=True)) + EPS) * pre_gain).astype(jnp.bfloat16)
    gate_low = gate_weight.astype(jnp.bfloat16)
    up_low = up_weight.astype(jnp.bfloat16)
    down_low = down_weight.astype(jnp.bfloat16)
    gate = jnp.dot(normed, gate_low, preferred_element_type=jnp.float32) * gate_scale
    up = jnp.dot(normed, up_low, preferred_element_type=jnp.float32) * up_scale
    hidden = (jax.nn.silu(gate) * up).astype(jnp.bfloat16)
    width = FF // N_TP
    hidden_blocks = jnp.transpose(hidden.reshape(hidden.shape[0], N_TP, width), (1, 0, 2))
    down_blocks = down_low.reshape(N_TP, width, down_low.shape[1])

    def accumulate(total, pair):
        part = jnp.dot(pair[0], pair[1], preferred_element_type=jnp.float32).astype(jnp.bfloat16)
        return (total + part.astype(jnp.float32), None)
    start = jnp.zeros((hidden.shape[0], down_low.shape[1]), jnp.float32)
    summed, unused = lax.scan(accumulate, start, (hidden_blocks, down_blocks))
    branch = summed * down_scale
    scaled = branch * lax.rsqrt(lax.optimization_barrier(jnp.mean(branch * branch, axis=-1, keepdims=True)) + EPS) * post_gain
    return scaled.astype(jnp.bfloat16)
```

```python
import jax
import jax.numpy as jnp
from jax import lax
from jax.experimental import pallas as pl
from jax.experimental.pallas import tpu as pltpu
from jax.sharding import PartitionSpec as P

EPS = 1e-06
LANES = 128
CORES = 2
ROWS = 128


def flat(z, t, n_fs, n_tp):
    return (z % n_fs) * n_tp + t


def patterns(n_fs, n_tp):
    enter, own, ring = ([], [], [])
    for z in range(n_fs):
        for t in range(n_tp):
            here = flat(z, t, n_fs, n_tp)
            if t % CORES == 0:
                enter.append((here, flat(z, t + 1, n_fs, n_tp)))
                own.append((here, flat(z + 1, t, n_fs, n_tp)))
                ring.append((here, flat(z + 1, t, n_fs, n_tp)))
            else:
                enter.append((here, flat(z + 1, t - 1, n_fs, n_tp)))
                ring.append((here, flat(z - 1, t, n_fs, n_tp)))
    return enter, own, ring


def finish_kernel(n_fs, place, mine, other, scale, gain, out):
    z, core = (place[0], place[1])
    slots = mine.shape[1] // LANES
    total = None
    branches = []
    for held, which in ((mine, core), (other, 1 - core)):
        for k in range(slots):
            slab = lax.rem(jnp.where(which == 0, z - 1 - k, z + k) + n_fs, n_fs)
            branch = held[:, k * LANES : (k + 1) * LANES].astype(jnp.float32) * scale[pl.ds(slab, 1), :]
            squares = branch * branch
            total = squares if total is None else total + squares
            branches.append((slab, branch))
    width = LANES * len(branches)
    norm = lax.rsqrt(jnp.sum(total, axis=-1, keepdims=True) / width + EPS)
    for slab, branch in branches:
        at = pl.multiple_of(slab * LANES, LANES)
        out[:, pl.ds(at, LANES)] = (branch * norm * gain[pl.ds(slab, 1), :]).astype(out.dtype)


def finish(place, mine, other, down_scale, post_gain, n_fs):
    rows, half = mine.shape
    block = pl.BlockSpec((ROWS, half), lambda i, place: (i, 0))
    vector = pl.BlockSpec((2 * half // LANES, LANES), lambda i, place: (0, 0))
    return pl.pallas_call(
        lambda *refs: finish_kernel(n_fs, *refs),
        grid_spec=pltpu.PrefetchScalarGridSpec(
            num_scalar_prefetch=1,
            grid=(rows // ROWS,),
            in_specs=[block, block, vector, vector],
            out_specs=pl.BlockSpec((ROWS, 2 * half), lambda i, place: (i, 0)),
        ),
        out_shape=jax.ShapeDtypeStruct((rows, 2 * half), jnp.bfloat16),
    )(place, mine, other, down_scale.reshape(-1, LANES), post_gain.reshape(-1, LANES))


def body(
    tokens,
    pre_gain,
    gate_weight,
    gate_scale,
    up_weight,
    up_scale,
    down_weight,
    down_scale,
    post_gain,
):
    n_fs, n_tp = (lax.axis_size("fs"), lax.axis_size("tp"))
    both = ("fs", "tp")
    z, t = (lax.axis_index("fs"), lax.axis_index("tp"))
    core = t % CORES
    enter, own_first, ring = patterns(n_fs, n_tp)
    partner = [(i, i ^ 1) for i in range(n_tp)]
    chips = [[x * CORES + c for x in range(n_tp // CORES)] for c in range(CORES)]
    n_chips = n_tp // CORES
    low = jnp.bfloat16
    units = gate_weight.shape[1]

    packed = jnp.concatenate(
        [gate_weight.astype(low).T, up_weight.astype(low).T, down_weight.astype(low)], axis=0
    )
    other0 = lax.ppermute(packed, both, enter)
    shifted = lax.ppermute(packed, both, own_first)
    own0 = jnp.where(core == 0, shifted, packed)

    rows = tokens.astype(jnp.float32)
    inverse = lax.rsqrt(jnp.mean(rows * rows, axis=-1, keepdims=True) + EPS)

    def normed_slab(k):
        slab = jnp.where(core == 0, z - 1 - k, z + k) % n_fs
        part = lax.dynamic_slice_in_dim(tokens, slab * LANES, LANES, axis=1).astype(jnp.float32)
        return (part * inverse * lax.dynamic_slice_in_dim(pre_gain, slab * LANES, LANES)).astype(low)

    def product(weights, k_normed):
        return lax.dot_general(
            weights, k_normed, (((1,), (1,)), ((), ())), preferred_element_type=jnp.float32
        )

    first_own, first_other = (own0[: 2 * units], other0[: 2 * units])
    down = jnp.concatenate([own0[2 * units :], other0[2 * units :]], axis=0)
    downs = [down]
    slab = normed_slab(0)
    sum_own, sum_other = (product(first_own, slab), product(first_other, slab))
    for k in range(1, n_fs // 2):
        first_own = lax.ppermute(first_own, both, ring)
        first_other = lax.ppermute(first_other, both, ring)
        down = lax.ppermute(down, both, ring)
        downs.append(down)
        slab = normed_slab(k)
        sum_other = sum_other + product(first_other, slab)
        sum_own = sum_own + product(first_own, slab)

    arrived = lax.ppermute(sum_other.astype(low), "tp", partner)
    sums = sum_own + arrived.astype(jnp.float32)
    gate = sums[:units] * gate_scale[:, None]
    up = sums[units:] * up_scale[:, None]
    hidden = (jax.nn.silu(gate) * up).astype(low)
    hidden = jnp.concatenate([hidden, lax.ppermute(hidden, "tp", partner)], axis=0)

    columns = jnp.concatenate(downs, axis=1)
    partial = lax.dot_general(
        hidden, columns, (((0,), (0,)), ((), ())), preferred_element_type=jnp.float32
    ).astype(low)
    n_rows, half = partial.shape
    parts = lax.all_to_all(
        partial.reshape(n_chips, n_rows // n_chips, half),
        "tp", 0, 0, axis_index_groups=chips, tiled=True,
    )
    summed = jnp.sum(parts.astype(jnp.float32), axis=0).astype(low)
    mine = lax.all_to_all(
        jnp.broadcast_to(summed, (n_chips, *summed.shape)),
        "tp", 0, 0, axis_index_groups=chips, tiled=True,
    ).reshape(n_rows, half)
    other = lax.ppermute(mine, "tp", partner)
    place = jnp.stack([z, core]).astype(jnp.int32)
    return finish(place, mine, other, down_scale, post_gain, n_fs)


def solution(mesh):
    in_specs = (
        P(("grp", "fs"), None),
        P(),
        P("fs", "tp"),
        P("tp"),
        P("fs", "tp"),
        P("tp"),
        P("tp", "fs"),
        P(),
        P(),
    )
    out_specs = P(("grp", "fs"), None)
    return jax.shard_map(body, mesh=mesh, in_specs=in_specs, out_specs=out_specs, check_vma=False)
```

```python
import jax
import jax.numpy as jnp
from jax import lax
from jax.experimental import pallas as pl
from jax.experimental.pallas import tpu as pltpu
from jax.sharding import PartitionSpec as P


EPS = 1e-06
LANES = 128
CORES = 2
ROWS = 64
CHUNKS = 1
FINISH_VMEM = 12 << 20
CHAINS = ("own", "other", "down")


def flat(z, t, n_fs, n_tp):
    return (z % n_fs) * n_tp + t


def patterns(n_fs, n_tp):
    enter, own, ring = ([], [], [])
    for z in range(n_fs):
        for t in range(n_tp):
            here = flat(z, t, n_fs, n_tp)
            if t % CORES == 0:
                enter.append((here, flat(z, t + 1, n_fs, n_tp)))
                own.append((here, flat(z + 1, t, n_fs, n_tp)))
                ring.append((here, flat(z + 1, t, n_fs, n_tp)))
            else:
                enter.append((here, flat(z + 1, t - 1, n_fs, n_tp)))
                ring.append((here, flat(z - 1, t, n_fs, n_tp)))
    return enter, own, ring


def finish_kernel(n_fs, place, mine, other, scale, gain, *outs):
    out = outs[-1]
    z, core = (place[0], place[1])
    slots = mine.shape[1] // LANES
    at_rows = pl.ds(pl.multiple_of(pl.program_id(0) * ROWS, ROWS), ROWS)
    total = None
    branches = []
    for held, which in ((mine, core), (other, 1 - core)):
        for k in range(slots):
            slab = lax.rem(jnp.where(which == 0, z - 1 - k, z + k) + n_fs, n_fs)
            branch = held[at_rows, k * LANES : (k + 1) * LANES].astype(jnp.float32)
            branch = branch * scale[pl.ds(slab, 1), :]
            squares = branch * branch
            total = squares if total is None else total + squares
            branches.append((slab, branch))
    width = LANES * len(branches)
    norm = lax.rsqrt(jnp.sum(total, axis=-1, keepdims=True) / width + EPS)
    for slab, branch in branches:
        at = pl.multiple_of(slab * LANES, LANES)
        out[:, pl.ds(at, LANES)] = (branch * norm * gain[pl.ds(slab, 1), :]).astype(out.dtype)


def finish(place, mine, other, scale, gain, n_fs, chunk, n_rows, done):
    rows, half = mine.shape
    first = chunk * rows // ROWS
    whole = pl.BlockSpec(memory_space=pltpu.VMEM)
    earlier = [] if done is None else [done]
    return pl.pallas_call(
        lambda *refs: finish_kernel(n_fs, *refs),
        grid_spec=pltpu.PrefetchScalarGridSpec(
            num_scalar_prefetch=1,
            grid=(rows // ROWS,),
            in_specs=[whole] * 4 + [pl.BlockSpec(memory_space=pl.ANY)] * len(earlier),
            out_specs=pl.BlockSpec((ROWS, 2 * half), lambda i, place: (first + i, 0)),
        ),
        out_shape=jax.ShapeDtypeStruct((n_rows, 2 * half), jnp.bfloat16),
        input_output_aliases={5: 0} if earlier else {},
        compiler_params=pltpu.CompilerParams(vmem_limit_bytes=FINISH_VMEM),
    )(place, mine, other, scale, gain, *earlier)


def body(
    tokens,
    pre_gain,
    gate_weight,
    gate_scale,
    up_weight,
    up_scale,
    down_weight,
    down_scale,
    post_gain,
):
    n_fs, n_tp = (lax.axis_size("fs"), lax.axis_size("tp"))
    both = ("fs", "tp")
    z, t = (lax.axis_index("fs"), lax.axis_index("tp"))
    core = t % CORES
    enter, own_first, ring = patterns(n_fs, n_tp)
    partner = [(i, i ^ 1) for i in range(n_tp)]
    chips = [[x * CORES + c for x in range(n_tp // CORES)] for c in range(CORES)]
    n_chips = n_tp // CORES
    low = jnp.bfloat16
    units = gate_weight.shape[1]

    packed = jnp.concatenate(
        [
            (gate_weight * gate_scale).astype(low).T,
            (up_weight * up_scale).astype(low).T,
            down_weight.astype(low),
        ],
        axis=0,
    )
    other0 = lax.ppermute(packed, both, enter)
    shifted = lax.ppermute(packed, both, own_first)
    own0 = jnp.where(core == 0, shifted, packed)

    rows = tokens.astype(jnp.float32)
    inverse = lax.rsqrt(jnp.mean(rows * rows, axis=-1, keepdims=True) + EPS)

    def normed_slab(k):
        slab = jnp.where(core == 0, z - 1 - k, z + k) % n_fs
        part = lax.dynamic_slice_in_dim(tokens, slab * LANES, LANES, axis=1).astype(jnp.float32)
        return (part * inverse * lax.dynamic_slice_in_dim(pre_gain, slab * LANES, LANES)).astype(low)

    def product(weights, k_normed):
        return lax.dot_general(
            weights, k_normed, (((1,), (1,)), ((), ())), preferred_element_type=jnp.float32
        )

    held = {
        "own": own0[: 2 * units],
        "other": other0[: 2 * units],
        "down": jnp.concatenate([own0[2 * units :], other0[2 * units :]], axis=0),
    }
    downs = [held["down"]]
    slab = normed_slab(0)
    sum_own, sum_other = (product(held["own"], slab), product(held["other"], slab))
    for k in range(1, n_fs // 2):
        for chain in CHAINS:
            held[chain] = lax.ppermute(held[chain], both, ring)
        downs.append(held["down"])
        slab = normed_slab(k)
        sum_own = sum_own + product(held["own"], slab)
        sum_other = sum_other + product(held["other"], slab)

    sums = jnp.concatenate([sum_own, sum_other], axis=0).astype(low)
    arrived = lax.ppermute(sums, "tp", partner)

    def gated(sums, more):
        sums = sums + more.astype(jnp.float32)
        return (jax.nn.silu(sums[:units]) * sums[units:]).astype(low)

    hidden = jnp.concatenate(
        [gated(sum_own, arrived[2 * units :]), gated(sum_other, arrived[: 2 * units])], axis=0
    )
    columns = jnp.concatenate(downs, axis=1)

    n_rows = tokens.shape[0]
    lines = n_rows // CHUNKS
    scale, gain = (down_scale.reshape(-1, LANES), post_gain.reshape(-1, LANES))
    place = jnp.stack([z, core]).astype(jnp.int32)

    def over_chips(array):
        return lax.all_to_all(array, "tp", 0, 0, axis_index_groups=chips, tiled=True)

    parts = []
    for c in range(CHUNKS):
        partial = lax.dot_general(
            hidden[:, c * lines : (c + 1) * lines],
            columns,
            (((0,), (0,)), ((), ())),
            preferred_element_type=jnp.float32,
        ).astype(low)
        parts.append(over_chips(partial.reshape(n_chips, lines // n_chips, -1)))
    mines = []
    for part in parts:
        summed = jnp.sum(part.astype(jnp.float32), axis=0).astype(low)
        mines.append(over_chips(jnp.broadcast_to(summed, part.shape)).reshape(lines, -1))
    out = None
    for c, mine in enumerate(mines):
        other = lax.ppermute(mine, "tp", partner)
        out = finish(place, mine, other, scale, gain, n_fs, c, n_rows, out)
    return out


def solution(mesh):
    in_specs = (
        P(("grp", "fs"), None),
        P(),
        P("fs", "tp"),
        P("tp"),
        P("fs", "tp"),
        P("tp"),
        P("tp", "fs"),
        P(),
        P(),
    )
    out_specs = P(("grp", "fs"), None)

    return jax.shard_map(body, mesh=mesh, in_specs=in_specs, out_specs=out_specs, check_vma=False)
```

```python
import jax
import jax.numpy as jnp
from jax import lax
from jax.experimental import pallas as pl
from jax.experimental.pallas import tpu as pltpu
from jax.sharding import PartitionSpec as P


EPS = 1e-06
LANES = 128
CORES = 2
ROWS = 64
CHUNKS = 1
FINISH_VMEM = 12 << 20
CHAINS = ("own", "other", "down")


def flat(z, t, n_fs, n_tp):
    return (z % n_fs) * n_tp + t


def patterns(n_fs, n_tp):
    enter, own, ring = ([], [], [])
    for z in range(n_fs):
        for t in range(n_tp):
            here = flat(z, t, n_fs, n_tp)
            if t % CORES == 0:
                enter.append((here, flat(z, t + 1, n_fs, n_tp)))
                own.append((here, flat(z - 1, t, n_fs, n_tp)))
                ring.append((here, flat(z - 1, t, n_fs, n_tp)))
            else:
                enter.append((here, flat(z - 1, t - 1, n_fs, n_tp)))
                ring.append((here, flat(z + 1, t, n_fs, n_tp)))
    return enter, own, ring


def slab_of(slot, core, z, n_fs):
    return lax.rem(jnp.where(core == 0, z + 1 + slot, z - slot + n_fs), n_fs)


def finish_kernel(n_fs, place, mine, other, scale, gain, *outs):
    out = outs[-1]
    z, core = (place[0], place[1])
    slots = mine.shape[1] // LANES
    at_rows = pl.ds(pl.multiple_of(pl.program_id(0) * ROWS, ROWS), ROWS)
    total = None
    branches = []
    for held, which in ((mine, core), (other, 1 - core)):
        for k in range(slots):
            slab = slab_of(k, which, z, n_fs)
            branch = held[at_rows, k * LANES : (k + 1) * LANES].astype(jnp.float32)
            branch = branch * scale[pl.ds(slab, 1), :]
            squares = branch * branch
            total = squares if total is None else total + squares
            branches.append((slab, branch))
    width = LANES * len(branches)
    norm = lax.rsqrt(jnp.sum(total, axis=-1, keepdims=True) / width + EPS)
    for slab, branch in branches:
        at = pl.multiple_of(slab * LANES, LANES)
        out[:, pl.ds(at, LANES)] = (branch * norm * gain[pl.ds(slab, 1), :]).astype(out.dtype)


def finish(place, mine, other, scale, gain, n_fs, chunk, n_rows, done):
    rows, half = mine.shape
    first = chunk * rows // ROWS
    whole = pl.BlockSpec(memory_space=pltpu.VMEM)
    earlier = [] if done is None else [done]
    return pl.pallas_call(
        lambda *refs: finish_kernel(n_fs, *refs),
        grid_spec=pltpu.PrefetchScalarGridSpec(
            num_scalar_prefetch=1,
            grid=(rows // ROWS,),
            in_specs=[whole] * 4 + [pl.BlockSpec(memory_space=pl.ANY)] * len(earlier),
            out_specs=pl.BlockSpec((ROWS, 2 * half), lambda i, place: (first + i, 0)),
        ),
        out_shape=jax.ShapeDtypeStruct((n_rows, 2 * half), jnp.bfloat16),
        input_output_aliases={5: 0} if earlier else {},
        compiler_params=pltpu.CompilerParams(vmem_limit_bytes=FINISH_VMEM),
    )(place, mine, other, scale, gain, *earlier)


def body(
    tokens,
    pre_gain,
    gate_weight,
    gate_scale,
    up_weight,
    up_scale,
    down_weight,
    down_scale,
    post_gain,
):
    n_fs, n_tp = (lax.axis_size("fs"), lax.axis_size("tp"))
    both = ("fs", "tp")
    z, t = (lax.axis_index("fs"), lax.axis_index("tp"))
    core = t % CORES
    enter, own_first, ring = patterns(n_fs, n_tp)
    partner = [(i, i ^ 1) for i in range(n_tp)]
    chips = [[x * CORES + c for x in range(n_tp // CORES)] for c in range(CORES)]
    n_chips = n_tp // CORES
    low = jnp.bfloat16
    units = gate_weight.shape[1]

    packed = jnp.concatenate(
        [
            (gate_weight * gate_scale).astype(low).T,
            (up_weight * up_scale).astype(low).T,
            down_weight.astype(low),
        ],
        axis=0,
    )
    other0 = lax.ppermute(packed, both, enter)
    shifted = lax.ppermute(packed, both, own_first)
    own0 = jnp.where(core == 0, shifted, packed)

    rows = tokens.astype(jnp.float32)
    inverse = lax.rsqrt(jnp.mean(rows * rows, axis=-1, keepdims=True) + EPS)

    def normed_slab(k):
        slab = slab_of(k, core, z, n_fs)
        part = lax.dynamic_slice_in_dim(tokens, slab * LANES, LANES, axis=1).astype(jnp.float32)
        return (part * inverse * lax.dynamic_slice_in_dim(pre_gain, slab * LANES, LANES)).astype(low)

    def product(weights, k_normed):
        return lax.dot_general(
            weights, k_normed, (((1,), (1,)), ((), ())), preferred_element_type=jnp.float32
        )

    held = {
        "own": own0[: 2 * units],
        "other": other0[: 2 * units],
        "down": jnp.concatenate([own0[2 * units :], other0[2 * units :]], axis=0),
    }
    downs = [held["down"]]
    slab = normed_slab(0)
    sum_own, sum_other = (product(held["own"], slab), product(held["other"], slab))
    for k in range(1, n_fs // 2):
        for chain in CHAINS:
            held[chain] = lax.ppermute(held[chain], both, ring)
        downs.append(held["down"])
        slab = normed_slab(k)
        sum_own = sum_own + product(held["own"], slab)
        sum_other = sum_other + product(held["other"], slab)

    sums = jnp.concatenate([sum_own, sum_other], axis=0).astype(low)
    arrived = lax.ppermute(sums, "tp", partner)

    def gated(sums, more):
        sums = sums + more.astype(jnp.float32)
        return (jax.nn.silu(sums[:units]) * sums[units:]).astype(low)

    hidden = jnp.concatenate(
        [gated(sum_own, arrived[2 * units :]), gated(sum_other, arrived[: 2 * units])], axis=0
    )
    columns = jnp.concatenate(downs, axis=1)

    n_rows = tokens.shape[0]
    lines = n_rows // CHUNKS
    scale, gain = (down_scale.reshape(-1, LANES), post_gain.reshape(-1, LANES))
    place = jnp.stack([z, core]).astype(jnp.int32)

    def over_chips(array):
        return lax.all_to_all(array, "tp", 0, 0, axis_index_groups=chips, tiled=True)

    parts = []
    for c in range(CHUNKS):
        partial = lax.dot_general(
            hidden[:, c * lines : (c + 1) * lines],
            columns,
            (((0,), (0,)), ((), ())),
            preferred_element_type=jnp.float32,
        ).astype(low)
        parts.append(over_chips(partial.reshape(n_chips, lines // n_chips, -1)))
    mines = []
    for part in parts:
        summed = jnp.sum(part.astype(jnp.float32), axis=0).astype(low)
        mines.append(over_chips(jnp.broadcast_to(summed, part.shape)).reshape(lines, -1))
    out = None
    for c, mine in enumerate(mines):
        other = lax.ppermute(mine, "tp", partner)
        out = finish(place, mine, other, scale, gain, n_fs, c, n_rows, out)
    return out


def solution(mesh):
    in_specs = (
        P(("grp", "fs"), None),
        P(),
        P("fs", "tp"),
        P("tp"),
        P("fs", "tp"),
        P("tp"),
        P("tp", "fs"),
        P(),
        P(),
    )
    out_specs = P(("grp", "fs"), None)

    return jax.shard_map(body, mesh=mesh, in_specs=in_specs, out_specs=out_specs, check_vma=False)
```

```python
import jax
import jax.numpy as jnp
from jax import lax
from jax.experimental import pallas as pl
from jax.experimental.pallas import tpu as pltpu
from jax.sharding import PartitionSpec as P


EPS = 1e-06
LANES = 128
CORES = 2
ROWS = 256
CHUNKS = 1
FINISH_VMEM = 12 << 20
CHAINS = ("own", "other")


def flat(z, t, n_fs, n_tp):
    return (z % n_fs) * n_tp + t


def patterns(n_fs, n_tp):
    enter, own, ring = ([], [], [])
    for z in range(n_fs):
        for t in range(n_tp):
            here = flat(z, t, n_fs, n_tp)
            if t % CORES == 0:
                enter.append((here, flat(z - 1, t + 1, n_fs, n_tp)))
                ring.append((here, flat(z + 1, t, n_fs, n_tp)))
            else:
                enter.append((here, flat(z, t - 1, n_fs, n_tp)))
                own.append((here, flat(z - 1, t, n_fs, n_tp)))
                ring.append((here, flat(z - 1, t, n_fs, n_tp)))
    return enter, own, ring


def slab_of(slot, core, z, n_fs):
    return lax.rem(jnp.where(core == 0, z - slot + n_fs, z + 1 + slot), n_fs)


def finish_kernel(n_fs, place, mine, other, scale, gain, *outs):
    out = outs[-1]
    z, core = (place[0], place[1])
    slots = mine.shape[1] // LANES
    at_rows = pl.ds(pl.multiple_of(pl.program_id(0) * ROWS, ROWS), ROWS)
    total = None
    branches = []
    for held, which in ((mine, core), (other, 1 - core)):
        for k in range(slots):
            slab = slab_of(k, which, z, n_fs)
            branch = held[at_rows, k * LANES : (k + 1) * LANES].astype(jnp.float32)
            branch = branch * scale[pl.ds(slab, 1), :]
            squares = branch * branch
            total = squares if total is None else total + squares
            branches.append((slab, branch))
    width = LANES * len(branches)
    norm = lax.rsqrt(jnp.sum(total, axis=-1, keepdims=True) / width + EPS)
    for slab, branch in branches:
        at = pl.multiple_of(slab * LANES, LANES)
        out[:, pl.ds(at, LANES)] = (branch * norm * gain[pl.ds(slab, 1), :]).astype(out.dtype)


def finish(place, mine, other, scale, gain, n_fs, chunk, n_rows, done):
    rows, half = mine.shape
    first = chunk * rows // ROWS
    whole = pl.BlockSpec(memory_space=pltpu.VMEM)
    earlier = [] if done is None else [done]
    return pl.pallas_call(
        lambda *refs: finish_kernel(n_fs, *refs),
        grid_spec=pltpu.PrefetchScalarGridSpec(
            num_scalar_prefetch=1,
            grid=(rows // ROWS,),
            in_specs=[whole] * 4 + [pl.BlockSpec(memory_space=pl.ANY)] * len(earlier),
            out_specs=pl.BlockSpec((ROWS, 2 * half), lambda i, place: (first + i, 0)),
        ),
        out_shape=jax.ShapeDtypeStruct((n_rows, 2 * half), jnp.bfloat16),
        input_output_aliases={5: 0} if earlier else {},
        compiler_params=pltpu.CompilerParams(vmem_limit_bytes=FINISH_VMEM),
    )(place, mine, other, scale, gain, *earlier)


def body(
    tokens,
    pre_gain,
    gate_weight,
    gate_scale,
    up_weight,
    up_scale,
    down_weight,
    down_scale,
    post_gain,
):
    n_fs, n_tp = (lax.axis_size("fs"), lax.axis_size("tp"))
    both = ("fs", "tp")
    z, t = (lax.axis_index("fs"), lax.axis_index("tp"))
    core = t % CORES
    enter, own_first, ring = patterns(n_fs, n_tp)
    partner = [(i, i ^ 1) for i in range(n_tp)]
    chips = [[x * CORES + c for x in range(n_tp // CORES)] for c in range(CORES)]
    n_chips = n_tp // CORES
    low = jnp.bfloat16
    units = gate_weight.shape[1]

    packed = jnp.concatenate(
        [
            (gate_weight * gate_scale).astype(low).T,
            (up_weight * up_scale).astype(low).T,
            down_weight.astype(low),
        ],
        axis=0,
    )
    other0 = lax.ppermute(packed, both, enter)
    shifted = lax.ppermute(packed, both, own_first)
    own0 = jnp.where(core == 0, packed, shifted)

    rows = tokens.astype(jnp.float32)
    inverse = lax.rsqrt(jnp.mean(rows * rows, axis=-1, keepdims=True) + EPS)

    def normed_slab(k):
        slab = slab_of(k, core, z, n_fs)
        part = lax.dynamic_slice_in_dim(tokens, slab * LANES, LANES, axis=1).astype(jnp.float32)
        return (part * inverse * lax.dynamic_slice_in_dim(pre_gain, slab * LANES, LANES)).astype(low)

    def product(weights, k_normed):
        return lax.dot_general(
            weights, k_normed, (((1,), (1,)), ((), ())), preferred_element_type=jnp.float32
        )

    held = {"own": own0, "other": other0}

    def down_rows():
        return jnp.concatenate([held["own"][2 * units :], held["other"][2 * units :]], axis=0)

    downs = [down_rows()]
    slab = normed_slab(0)
    sum_own, sum_other = (product(held["own"][: 2 * units], slab), product(held["other"][: 2 * units], slab))
    for k in range(1, n_fs // 2):
        for chain in CHAINS:
            held[chain] = lax.ppermute(held[chain], both, ring)
        downs.append(down_rows())
        slab = normed_slab(k)
        sum_own = sum_own + product(held["own"][: 2 * units], slab)
        sum_other = sum_other + product(held["other"][: 2 * units], slab)

    sums = jnp.concatenate([sum_own, sum_other], axis=0).astype(low)
    arrived = lax.ppermute(sums, "tp", partner)

    def gated(sums, more):
        sums = sums + more.astype(jnp.float32)
        return (jax.nn.silu(sums[:units]) * sums[units:]).astype(low)

    hidden = jnp.concatenate(
        [gated(sum_own, arrived[2 * units :]), gated(sum_other, arrived[: 2 * units])], axis=0
    )
    columns = jnp.concatenate(downs, axis=1)

    n_rows = tokens.shape[0]
    lines = n_rows // CHUNKS
    scale, gain = (down_scale.reshape(-1, LANES), post_gain.reshape(-1, LANES))
    place = jnp.stack([z, core]).astype(jnp.int32)

    def over_chips(array):
        return lax.all_to_all(array, "tp", 0, 0, axis_index_groups=chips, tiled=True)

    parts = []
    for c in range(CHUNKS):
        partial = lax.dot_general(
            hidden[:, c * lines : (c + 1) * lines],
            columns,
            (((0,), (0,)), ((), ())),
            preferred_element_type=jnp.float32,
        ).astype(low)
        parts.append(over_chips(partial.reshape(n_chips, lines // n_chips, -1)))
    mines = []
    for part in parts:
        summed = jnp.sum(part.astype(jnp.float32), axis=0).astype(low)
        mines.append(over_chips(jnp.broadcast_to(summed, part.shape)).reshape(lines, -1))
    out = None
    for c, mine in enumerate(mines):
        other = lax.ppermute(mine, "tp", partner)
        out = finish(place, mine, other, scale, gain, n_fs, c, n_rows, out)
    return out


def solution(mesh):
    in_specs = (
        P(("grp", "fs"), None),
        P(),
        P("fs", "tp"),
        P("tp"),
        P("fs", "tp"),
        P("tp"),
        P("tp", "fs"),
        P(),
        P(),
    )
    out_specs = P(("grp", "fs"), None)

    return jax.shard_map(body, mesh=mesh, in_specs=in_specs, out_specs=out_specs, check_vma=False)
```

```python
import jax
import jax.numpy as jnp
from jax import lax
from jax.experimental import pallas as pl
from jax.experimental.pallas import tpu as pltpu
from jax.sharding import PartitionSpec as P


EPS = 1e-06
LANES = 128
CORES = 2
ROWS = 256
CHUNKS = 1
FINISH_VMEM = 12 << 20
WHOLE = 3


def flat(z, t, n_fs, n_tp):
    return (z % n_fs) * n_tp + t


def patterns(n_fs, n_tp):
    enter, own, ring = ([], [], [])
    for z in range(n_fs):
        for t in range(n_tp):
            here = flat(z, t, n_fs, n_tp)
            if t % CORES == 0:
                enter.append((here, flat(z - 1, t + 1, n_fs, n_tp)))
                ring.append((here, flat(z + 1, t, n_fs, n_tp)))
            else:
                enter.append((here, flat(z, t - 1, n_fs, n_tp)))
                own.append((here, flat(z - 1, t, n_fs, n_tp)))
                ring.append((here, flat(z - 1, t, n_fs, n_tp)))
    return enter, own, ring


def chains_of(k):
    return ("own", "other") if k <= WHOLE else ("own", "other", "down")


def slab_of(slot, core, z, n_fs):
    return lax.rem(jnp.where(core == 0, z - slot + n_fs, z + 1 + slot), n_fs)


def finish_kernel(n_fs, place, mine, other, scale, gain, *outs):
    out = outs[-1]
    z, core = (place[0], place[1])
    slots = mine.shape[1] // LANES
    at_rows = pl.ds(pl.multiple_of(pl.program_id(0) * ROWS, ROWS), ROWS)
    total = None
    branches = []
    for held, which in ((mine, core), (other, 1 - core)):
        for k in range(slots):
            slab = slab_of(k, which, z, n_fs)
            branch = held[at_rows, k * LANES : (k + 1) * LANES].astype(jnp.float32)
            branch = branch * scale[pl.ds(slab, 1), :]
            squares = branch * branch
            total = squares if total is None else total + squares
            branches.append((slab, branch))
    width = LANES * len(branches)
    norm = lax.rsqrt(jnp.sum(total, axis=-1, keepdims=True) / width + EPS)
    for slab, branch in branches:
        at = pl.multiple_of(slab * LANES, LANES)
        out[:, pl.ds(at, LANES)] = (branch * norm * gain[pl.ds(slab, 1), :]).astype(out.dtype)


def finish(place, mine, other, scale, gain, n_fs, chunk, n_rows, done):
    rows, half = mine.shape
    first = chunk * rows // ROWS
    whole = pl.BlockSpec(memory_space=pltpu.VMEM)
    earlier = [] if done is None else [done]
    return pl.pallas_call(
        lambda *refs: finish_kernel(n_fs, *refs),
        grid_spec=pltpu.PrefetchScalarGridSpec(
            num_scalar_prefetch=1,
            grid=(rows // ROWS,),
            in_specs=[whole] * 4 + [pl.BlockSpec(memory_space=pl.ANY)] * len(earlier),
            out_specs=pl.BlockSpec((ROWS, 2 * half), lambda i, place: (first + i, 0)),
        ),
        out_shape=jax.ShapeDtypeStruct((n_rows, 2 * half), jnp.bfloat16),
        input_output_aliases={5: 0} if earlier else {},
        compiler_params=pltpu.CompilerParams(vmem_limit_bytes=FINISH_VMEM),
    )(place, mine, other, scale, gain, *earlier)


def body(
    tokens,
    pre_gain,
    gate_weight,
    gate_scale,
    up_weight,
    up_scale,
    down_weight,
    down_scale,
    post_gain,
):
    n_fs, n_tp = (lax.axis_size("fs"), lax.axis_size("tp"))
    both = ("fs", "tp")
    z, t = (lax.axis_index("fs"), lax.axis_index("tp"))
    core = t % CORES
    enter, own_first, ring = patterns(n_fs, n_tp)
    partner = [(i, i ^ 1) for i in range(n_tp)]
    chips = [[x * CORES + c for x in range(n_tp // CORES)] for c in range(CORES)]
    n_chips = n_tp // CORES
    low = jnp.bfloat16
    units = gate_weight.shape[1]

    packed = jnp.concatenate(
        [
            (gate_weight * gate_scale).astype(low).T,
            (up_weight * up_scale).astype(low).T,
            down_weight.astype(low),
        ],
        axis=0,
    )
    other0 = lax.ppermute(packed, both, enter)
    shifted = lax.ppermute(packed, both, own_first)
    own0 = jnp.where(core == 0, packed, shifted)

    rows = tokens.astype(jnp.float32)
    inverse = lax.rsqrt(jnp.mean(rows * rows, axis=-1, keepdims=True) + EPS)

    def normed_slab(k):
        slab = slab_of(k, core, z, n_fs)
        part = lax.dynamic_slice_in_dim(tokens, slab * LANES, LANES, axis=1).astype(jnp.float32)
        return (part * inverse * lax.dynamic_slice_in_dim(pre_gain, slab * LANES, LANES)).astype(low)

    def product(weights, k_normed):
        return lax.dot_general(
            weights, k_normed, (((1,), (1,)), ((), ())), preferred_element_type=jnp.float32
        )

    held = {"own": own0, "other": other0}

    def down_rows():
        return jnp.concatenate([held["own"][2 * units :], held["other"][2 * units :]], axis=0)

    downs = [down_rows()]
    slab = normed_slab(0)
    sum_own, sum_other = (product(held["own"][: 2 * units], slab), product(held["other"][: 2 * units], slab))
    for k in range(1, n_fs // 2):
        if k == WHOLE + 1:
            held = {"own": held["own"][: 2 * units], "other": held["other"][: 2 * units], "down": downs[-1]}
        for chain in chains_of(k):
            held[chain] = lax.ppermute(held[chain], both, ring)
        downs.append(down_rows() if k <= WHOLE else held["down"])
        slab = normed_slab(k)
        sum_own = sum_own + product(held["own"][: 2 * units], slab)
        sum_other = sum_other + product(held["other"][: 2 * units], slab)

    sums = jnp.concatenate([sum_own, sum_other], axis=0).astype(low)
    arrived = lax.ppermute(sums, "tp", partner)

    def gated(sums, more):
        gate = sums[:units] + more[:units].astype(jnp.float32)
        up = sums[units:] + more[units:].astype(jnp.float32)
        return (jax.nn.silu(gate) * up).astype(low)

    hidden = jnp.concatenate(
        [gated(sum_own, arrived[2 * units :]), gated(sum_other, arrived[: 2 * units])], axis=0
    )
    columns = jnp.concatenate(downs, axis=1)

    n_rows = tokens.shape[0]
    lines = n_rows // CHUNKS
    scale, gain = (down_scale.reshape(-1, LANES), post_gain.reshape(-1, LANES))
    place = jnp.stack([z, core]).astype(jnp.int32)

    def over_chips(array):
        return lax.all_to_all(array, "tp", 0, 0, axis_index_groups=chips, tiled=True)

    parts = []
    for c in range(CHUNKS):
        partial = lax.dot_general(
            hidden[:, c * lines : (c + 1) * lines],
            columns,
            (((0,), (0,)), ((), ())),
            preferred_element_type=jnp.float32,
        ).astype(low)
        parts.append(over_chips(partial.reshape(n_chips, lines // n_chips, -1)))
    mines = []
    for part in parts:
        summed = jnp.sum(part.astype(jnp.float32), axis=0).astype(low)
        mines.append(over_chips(jnp.broadcast_to(summed, part.shape)).reshape(lines, -1))
    out = None
    for c, mine in enumerate(mines):
        other = lax.ppermute(mine, "tp", partner)
        out = finish(place, mine, other, scale, gain, n_fs, c, n_rows, out)
    return out


def solution(mesh):
    in_specs = (
        P(("grp", "fs"), None),
        P(),
        P("fs", "tp"),
        P("tp"),
        P("fs", "tp"),
        P("tp"),
        P("tp", "fs"),
        P(),
        P(),
    )
    out_specs = P(("grp", "fs"), None)

    return jax.shard_map(body, mesh=mesh, in_specs=in_specs, out_specs=out_specs, check_vma=False)
```

```python
import jax
import jax.numpy as jnp
from jax import lax
from jax.experimental import pallas as pl
from jax.experimental.pallas import tpu as pltpu
from jax.sharding import PartitionSpec as P


EPS = 1e-06
LANES = 128
CORES = 2
ROWS = 256
CHUNKS = 1
FINISH_VMEM = 12 << 20
CHAINS = ("own", "other")


def flat(z, t, n_fs, n_tp):
    return (z % n_fs) * n_tp + t


def patterns(n_fs, n_tp):
    enter, own, ring = ([], [], [])
    for z in range(n_fs):
        for t in range(n_tp):
            here = flat(z, t, n_fs, n_tp)
            if t % CORES == 0:
                enter.append((here, flat(z - 1, t + 1, n_fs, n_tp)))
                ring.append((here, flat(z + 1, t, n_fs, n_tp)))
            else:
                enter.append((here, flat(z, t - 1, n_fs, n_tp)))
                own.append((here, flat(z - 1, t, n_fs, n_tp)))
                ring.append((here, flat(z - 1, t, n_fs, n_tp)))
    return enter, own, ring


def slab_of(slot, core, z, n_fs):
    return lax.rem(jnp.where(core == 0, z - slot + n_fs, z + 1 + slot), n_fs)


def finish_kernel(n_fs, place, mine, other, scale, gain, *outs):
    out = outs[-1]
    z, core = (place[0], place[1])
    slots = mine.shape[1] // LANES
    at_rows = pl.ds(pl.multiple_of(pl.program_id(0) * ROWS, ROWS), ROWS)
    total = None
    branches = []
    for held, which in ((mine, core), (other, 1 - core)):
        for k in range(slots):
            slab = slab_of(k, which, z, n_fs)
            branch = held[at_rows, k * LANES : (k + 1) * LANES].astype(jnp.float32)
            branch = branch * scale[pl.ds(slab, 1), :]
            squares = branch * branch
            total = squares if total is None else total + squares
            branches.append((slab, branch))
    width = LANES * len(branches)
    norm = lax.rsqrt(jnp.sum(total, axis=-1, keepdims=True) / width + EPS)
    for slab, branch in branches:
        at = pl.multiple_of(slab * LANES, LANES)
        out[:, pl.ds(at, LANES)] = (branch * norm * gain[pl.ds(slab, 1), :]).astype(out.dtype)


def finish(place, mine, other, scale, gain, n_fs, chunk, n_rows, done):
    rows, half = mine.shape
    first = chunk * rows // ROWS
    whole = pl.BlockSpec(memory_space=pltpu.VMEM)
    earlier = [] if done is None else [done]
    return pl.pallas_call(
        lambda *refs: finish_kernel(n_fs, *refs),
        grid_spec=pltpu.PrefetchScalarGridSpec(
            num_scalar_prefetch=1,
            grid=(rows // ROWS,),
            in_specs=[whole] * 4 + [pl.BlockSpec(memory_space=pl.ANY)] * len(earlier),
            out_specs=pl.BlockSpec((ROWS, 2 * half), lambda i, place: (first + i, 0)),
        ),
        out_shape=jax.ShapeDtypeStruct((n_rows, 2 * half), jnp.bfloat16),
        input_output_aliases={5: 0} if earlier else {},
        compiler_params=pltpu.CompilerParams(vmem_limit_bytes=FINISH_VMEM),
    )(place, mine, other, scale, gain, *earlier)


def body(
    tokens,
    pre_gain,
    gate_weight,
    gate_scale,
    up_weight,
    up_scale,
    down_weight,
    down_scale,
    post_gain,
):
    n_fs, n_tp = (lax.axis_size("fs"), lax.axis_size("tp"))
    both = ("fs", "tp")
    z, t = (lax.axis_index("fs"), lax.axis_index("tp"))
    core = t % CORES
    enter, own_first, ring = patterns(n_fs, n_tp)
    partner = [(i, i ^ 1) for i in range(n_tp)]
    chips = [[x * CORES + c for x in range(n_tp // CORES)] for c in range(CORES)]
    n_chips = n_tp // CORES
    low = jnp.bfloat16
    units = gate_weight.shape[1]

    packed = jnp.concatenate(
        [
            (gate_weight * gate_scale).astype(low).T,
            (up_weight * up_scale).astype(low).T,
            down_weight.astype(low),
        ],
        axis=0,
    )
    other0 = lax.ppermute(packed, both, enter)
    shifted = lax.ppermute(packed, both, own_first)
    own0 = jnp.where(core == 0, packed, shifted)

    rows = tokens.astype(jnp.float32)
    inverse = lax.rsqrt(jnp.mean(rows * rows, axis=-1, keepdims=True) + EPS)

    def normed_slab(k):
        slab = slab_of(k, core, z, n_fs)
        part = lax.dynamic_slice_in_dim(tokens, slab * LANES, LANES, axis=1).astype(jnp.float32)
        return (part * inverse * lax.dynamic_slice_in_dim(pre_gain, slab * LANES, LANES)).astype(low)

    def product(weights, k_normed):
        return lax.dot_general(
            weights, k_normed, (((1,), (1,)), ((), ())), preferred_element_type=jnp.float32
        )

    held = {"own": own0, "other": other0}

    def down_rows():
        return jnp.concatenate([held["own"][2 * units :], held["other"][2 * units :]], axis=0)

    downs = [down_rows()]
    slab = normed_slab(0)
    sum_own, sum_other = (product(held["own"][: 2 * units], slab), product(held["other"][: 2 * units], slab))
    for k in range(1, n_fs // 2):
        for chain in CHAINS:
            held[chain] = lax.ppermute(held[chain], both, ring)
        downs.append(down_rows())
        slab = normed_slab(k)
        sum_own = sum_own + product(held["own"][: 2 * units], slab)
        sum_other = sum_other + product(held["other"][: 2 * units], slab)

    for_other = lax.ppermute(sum_own.astype(low), "tp", partner)
    for_own = lax.ppermute(sum_other.astype(low), "tp", partner)

    def gated(sums, more):
        gate = sums[:units] + more[:units].astype(jnp.float32)
        up = sums[units:] + more[units:].astype(jnp.float32)
        return (jax.nn.silu(gate) * up).astype(low)

    hidden = jnp.concatenate([gated(sum_own, for_own), gated(sum_other, for_other)], axis=0)
    columns = jnp.concatenate(downs, axis=1)

    n_rows = tokens.shape[0]
    lines = n_rows // CHUNKS
    scale, gain = (down_scale.reshape(-1, LANES), post_gain.reshape(-1, LANES))
    place = jnp.stack([z, core]).astype(jnp.int32)

    def over_chips(array):
        return lax.all_to_all(array, "tp", 0, 0, axis_index_groups=chips, tiled=True)

    parts = []
    for c in range(CHUNKS):
        partial = lax.dot_general(
            hidden[:, c * lines : (c + 1) * lines],
            columns,
            (((0,), (0,)), ((), ())),
            preferred_element_type=jnp.float32,
        ).astype(low)
        parts.append(over_chips(partial.reshape(n_chips, lines // n_chips, -1)))
    mines = []
    for part in parts:
        summed = jnp.sum(part.astype(jnp.float32), axis=0).astype(low)
        mines.append(over_chips(jnp.broadcast_to(summed, part.shape)).reshape(lines, -1))
    out = None
    for c, mine in enumerate(mines):
        other = lax.ppermute(mine, "tp", partner)
        out = finish(place, mine, other, scale, gain, n_fs, c, n_rows, out)
    return out


def solution(mesh):
    in_specs = (
        P(("grp", "fs"), None),
        P(),
        P("fs", "tp"),
        P("tp"),
        P("fs", "tp"),
        P("tp"),
        P("tp", "fs"),
        P(),
        P(),
    )
    out_specs = P(("grp", "fs"), None)

    return jax.shard_map(body, mesh=mesh, in_specs=in_specs, out_specs=out_specs, check_vma=False)
```

```python
import jax
import jax.numpy as jnp
from jax import lax
from jax.experimental import pallas as pl
from jax.experimental.pallas import tpu as pltpu
from jax.sharding import PartitionSpec as P


EPS = 1e-06
LANES = 128
CORES = 2
ROWS = 256
CHUNKS = 1
FINISH_VMEM = 12 << 20
CHAINS = ("own", "other")


def flat(z, t, n_fs, n_tp):
    return (z % n_fs) * n_tp + t


def patterns(n_fs, n_tp):
    enter, own, ring = ([], [], [])
    for z in range(n_fs):
        for t in range(n_tp):
            here = flat(z, t, n_fs, n_tp)
            if t % CORES == 0:
                enter.append((here, flat(z - 1, t + 1, n_fs, n_tp)))
                ring.append((here, flat(z + 1, t, n_fs, n_tp)))
            else:
                enter.append((here, flat(z, t - 1, n_fs, n_tp)))
                own.append((here, flat(z - 1, t, n_fs, n_tp)))
                ring.append((here, flat(z - 1, t, n_fs, n_tp)))
    return enter, own, ring


def slab_of(slot, core, z, n_fs):
    return lax.rem(jnp.where(core == 0, z - slot + n_fs, z + 1 + slot), n_fs)


def finish_kernel(n_fs, place, mine, other, scale, gain, *outs):
    out = outs[-1]
    z, core = (place[0], place[1])
    slots = mine.shape[1] // LANES
    at_rows = pl.ds(pl.multiple_of(pl.program_id(0) * ROWS, ROWS), ROWS)
    total = None
    branches = []
    for held, which in ((mine, core), (other, 1 - core)):
        for k in range(slots):
            slab = slab_of(k, which, z, n_fs)
            branch = held[at_rows, k * LANES : (k + 1) * LANES].astype(jnp.float32)
            branch = branch * scale[pl.ds(slab, 1), :]
            squares = branch * branch
            total = squares if total is None else total + squares
            branches.append((slab, branch))
    width = LANES * len(branches)
    norm = lax.rsqrt(jnp.sum(total, axis=-1, keepdims=True) / width + EPS)
    for slab, branch in branches:
        at = pl.multiple_of(slab * LANES, LANES)
        out[:, pl.ds(at, LANES)] = (branch * norm * gain[pl.ds(slab, 1), :]).astype(out.dtype)


def finish(place, mine, other, scale, gain, n_fs, chunk, n_rows, done):
    rows, half = mine.shape
    first = chunk * rows // ROWS
    whole = pl.BlockSpec(memory_space=pltpu.VMEM)
    earlier = [] if done is None else [done]
    return pl.pallas_call(
        lambda *refs: finish_kernel(n_fs, *refs),
        grid_spec=pltpu.PrefetchScalarGridSpec(
            num_scalar_prefetch=1,
            grid=(rows // ROWS,),
            in_specs=[whole] * 4 + [pl.BlockSpec(memory_space=pl.ANY)] * len(earlier),
            out_specs=pl.BlockSpec((ROWS, 2 * half), lambda i, place: (first + i, 0)),
        ),
        out_shape=jax.ShapeDtypeStruct((n_rows, 2 * half), jnp.bfloat16),
        input_output_aliases={5: 0} if earlier else {},
        compiler_params=pltpu.CompilerParams(vmem_limit_bytes=FINISH_VMEM),
    )(place, mine, other, scale, gain, *earlier)


def body(
    tokens,
    pre_gain,
    gate_weight,
    gate_scale,
    up_weight,
    up_scale,
    down_weight,
    down_scale,
    post_gain,
):
    n_fs, n_tp = (lax.axis_size("fs"), lax.axis_size("tp"))
    both = ("fs", "tp")
    z, t = (lax.axis_index("fs"), lax.axis_index("tp"))
    core = t % CORES
    enter, own_first, ring = patterns(n_fs, n_tp)
    partner = [(i, i ^ 1) for i in range(n_tp)]
    chips = [[x * CORES + c for x in range(n_tp // CORES)] for c in range(CORES)]
    n_chips = n_tp // CORES
    low = jnp.bfloat16
    units = gate_weight.shape[1]

    packed = jnp.concatenate(
        [
            (gate_weight * gate_scale).astype(low).T,
            (up_weight * up_scale).astype(low).T,
            down_weight.astype(low),
        ],
        axis=0,
    )
    other0 = lax.ppermute(packed, both, enter)
    shifted = lax.ppermute(packed, both, own_first)
    own0 = jnp.where(core == 0, packed, shifted)

    rows = tokens.astype(jnp.float32)
    inverse = lax.rsqrt(jnp.mean(rows * rows, axis=-1, keepdims=True) + EPS)

    def normed_slab(k):
        slab = slab_of(k, core, z, n_fs)
        part = lax.dynamic_slice_in_dim(tokens, slab * LANES, LANES, axis=1).astype(jnp.float32)
        return (part * inverse * lax.dynamic_slice_in_dim(pre_gain, slab * LANES, LANES)).astype(low)

    def product(weights, k_normed):
        return lax.dot_general(
            weights, k_normed, (((1,), (1,)), ((), ())), preferred_element_type=jnp.float32
        )

    held = {"own": own0, "other": other0}

    def down_rows():
        return jnp.concatenate([held["own"][2 * units :], held["other"][2 * units :]], axis=0)

    downs = [down_rows()]
    slab = normed_slab(0)
    sum_own, sum_other = (product(held["own"][: 2 * units], slab), product(held["other"][: 2 * units], slab))
    for k in range(1, n_fs // 2):
        for chain in CHAINS:
            held[chain] = lax.ppermute(held[chain], both, ring)
        downs.append(down_rows())
        slab = normed_slab(k)
        sum_own = sum_own + product(held["own"][: 2 * units], slab)
        sum_other = sum_other + product(held["other"][: 2 * units], slab)

    sums = jnp.concatenate([sum_own, sum_other], axis=0).astype(low)
    arrived = lax.ppermute(sums, "tp", partner)

    def gated(sums, more):
        gate = sums[:units] + more[:units].astype(jnp.float32)
        up = sums[units:] + more[units:].astype(jnp.float32)
        return (jax.nn.silu(gate) * up).astype(low)

    hidden = jnp.concatenate(
        [gated(sum_own, arrived[2 * units :]), gated(sum_other, arrived[: 2 * units])], axis=0
    )
    columns = jnp.concatenate(downs, axis=1)

    n_rows = tokens.shape[0]
    lines = n_rows // CHUNKS
    scale, gain = (down_scale.reshape(-1, LANES), post_gain.reshape(-1, LANES))
    place = jnp.stack([z, core]).astype(jnp.int32)

    def over_chips(array):
        return lax.all_to_all(array, "tp", 0, 0, axis_index_groups=chips, tiled=True)

    parts = []
    for c in range(CHUNKS):
        partial = lax.dot_general(
            hidden[:, c * lines : (c + 1) * lines],
            columns,
            (((0,), (0,)), ((), ())),
            preferred_element_type=jnp.float32,
        ).astype(low)
        parts.append(over_chips(partial.reshape(n_chips, lines // n_chips, -1)))
    mines = []
    for part in parts:
        summed = jnp.sum(part.astype(jnp.float32), axis=0).astype(low)
        mines.append(over_chips(jnp.broadcast_to(summed, part.shape)).reshape(lines, -1))
    out = None
    for c, mine in enumerate(mines):
        other = lax.ppermute(mine, "tp", partner)
        out = finish(place, mine, other, scale, gain, n_fs, c, n_rows, out)
    return out


def solution(mesh):
    in_specs = (
        P(("grp", "fs"), None),
        P(),
        P("fs", "tp"),
        P("tp"),
        P("fs", "tp"),
        P("tp"),
        P("tp", "fs"),
        P(),
        P(),
    )
    out_specs = P(("grp", "fs"), None)

    return jax.shard_map(body, mesh=mesh, in_specs=in_specs, out_specs=out_specs, check_vma=False)
```
